256 devices in a mesh: sp: 64 (over z, x, core), tp: 4 (over y).
Axes of the slice: x: 4, y: 4, z: 8, core: 2. Of those that a mesh axis runs over, the one named last changes fastest.
Arguments:
- query_logits: bfloat16 [32768, 4096], P('sp', 'tp'), may hold values from -6 to 6
- forget_logits: bfloat16 [32768, 4096], P('sp', 'tp'), may hold values from -6 to 6
- value_inputs: bfloat16 [32768, 4096], P('sp', 'tp'), may hold values from -16 to 16
- output_gate_logits: bfloat16 [32768, 4096], P('sp', 'tp'), may hold values from -6 to 6
- forget_floor_gap: float32 [4096], replicated, may hold values from 3.0517578e-06 to 0.1
- surge_log_decay: float32 [32, 32768], P('tp', 'sp'), may hold values from -0.7 to 0
- head_norm_gain: float32 [128], replicated, may hold values from 0.1 to 1.9
- output_matrix: bfloat16 [4096, 4096], P('sp', 'tp'), may hold values from -1.25 to 1.25
- branch_norm_gain: float32 [4096], replicated, may hold values from 0.1 to 1.9
- residual: bfloat16 [32768, 4096], P('sp', 'tp'), may hold values from -6 to 6
Outputs:
- output: bfloat16 [32768, 4096], P('sp', 'tp')
The draws below stay inside these ranges and needn't reach their ends.
All inputs are finite; a program needn't handle non-finite values.
Results may differ from the reference program's by a relative error of at most 0.005.
Values may be sent and summed in bfloat16 or wider, within the bound.
A program may use at most 128 MiB of HBM per device.

```python
import math
import jax
import jax.numpy as jnp
from jax import lax

HEAD_DIM = 128
HEAD_TOTAL = 32
D = 4096
BLOCK_SPAN = 64
TOK_DEV = 512
TOKEN_TOTAL = 32768


surge_count = 3


def draw_forget_logits(key, part):
    leading_item, second = jax.random.split(key, 2)
    width = HEAD_TOTAL * HEAD_DIM
    offsets = jax.random.uniform(second, (TOKEN_TOTAL // TOK_DEV, 1, 1), jnp.float32, -1.5, 1.5)
    base = jnp.clip(jax.random.normal(leading_item, (TOKEN_TOTAL, width), jnp.float32), -4.0, 4.0)
    shifted = base.reshape(TOKEN_TOTAL // TOK_DEV, TOK_DEV, width) + offsets
    return shifted.reshape(TOKEN_TOTAL, width).astype(jnp.bfloat16)


def draw_forget_floor_gap(key, part):
    leading_item, second, third = jax.random.split(key, 3)
    share = 0.5
    quick = jax.random.uniform(leading_item, (HEAD_TOTAL, 1), jnp.float32) < share
    slow_gap = jax.random.uniform(second, (HEAD_TOTAL, HEAD_DIM), jnp.float32, 0.1, 0.6) / TOKEN_TOTAL
    quick_gap = jnp.exp(jax.random.uniform(third, (HEAD_TOTAL, HEAD_DIM), jnp.float32, math.log(0.03), math.log(0.1)))
    return jnp.where(quick, quick_gap, slow_gap).reshape(HEAD_TOTAL * HEAD_DIM)


def draw_surge_log_decay(key, part):
    leading_item, second = jax.random.split(key, 2)
    position_grid = jax.random.randint(leading_item, (HEAD_TOTAL, surge_count), 0, TOKEN_TOTAL)
    hits = jnp.any(jnp.arange(TOKEN_TOTAL)[None, :, None] == position_grid[:, None, :], axis=2)
    amounts = jnp.log(jax.random.uniform(second, (HEAD_TOTAL, TOKEN_TOTAL), jnp.float32, 0.5, 0.8))
    return jnp.where(hits, amounts, 0.0).astype(jnp.float32)


def draw_output_matrix(key, part):
    leading_item, second = jax.random.split(key, 2)
    width = HEAD_TOTAL * HEAD_DIM
    limit = 80.0 / math.sqrt(width)
    ramp = jnp.exp(math.log(3.0) * jnp.arange(D).astype(jnp.float32) / D)
    base = jnp.clip(jax.random.normal(leading_item, (width, D), jnp.float32), -4.0, 4.0)
    column_scale = ramp * jnp.exp(jax.random.uniform(second, (D,), jnp.float32, 0.0, math.log(4.0)))
    values = jnp.clip(base * column_scale / math.sqrt(width), -limit, limit)
    return values.astype(jnp.bfloat16)


def shard_levels(key, extent, cuts, least, top_value):
    def one(dim, parts):
        draws = jax.random.uniform(jax.random.fold_in(jax.random.fold_in(key, 6), dim), (parts,), jnp.float32, least / len(cuts), top_value / len(cuts))
        return jnp.repeat(jnp.exp(draws), extent[dim] // parts).reshape((-1,) + (1,) * (len(extent) - dim - 1))

    loudness = one(*cuts[0])
    for cut in cuts[1:]:
        loudness = loudness * one(*cut)
    return loudness


def noise(own_key, dims, deviation, reach, cuts=(), kind=jnp.bfloat16):
    values = jax.random.normal(own_key, dims, jnp.float32) * deviation
    if len(cuts) > 0:
        values = shard_levels(own_key, dims, cuts, -0.22, 0.18) * values
    return jnp.clip(values, min=-reach, max=reach).astype(kind)


def setup_inputs(seed: int = 0) -> dict:
    arg_keys = jax.random.split(jax.random.key(seed), 11)
    return {
        "query_logits": noise(arg_keys[0], (TOKEN_TOTAL, HEAD_TOTAL * HEAD_DIM), 1.0, 6.0, ((0, 64), (1, 4))),
        "forget_logits": draw_forget_logits(jax.random.fold_in(arg_keys[10], 71), 0),
        "value_inputs": noise(arg_keys[2], (TOKEN_TOTAL, HEAD_TOTAL * HEAD_DIM), 4.0, 16.0, ((0, 64), (1, 4))),
        "output_gate_logits": noise(arg_keys[3], (TOKEN_TOTAL, HEAD_TOTAL * HEAD_DIM), 1.0, 6.0, ((0, 64), (1, 4))),
        "forget_floor_gap": draw_forget_floor_gap(jax.random.fold_in(arg_keys[10], 71), 0),
        "surge_log_decay": draw_surge_log_decay(jax.random.fold_in(arg_keys[10], 71), 0),
        "head_norm_gain": jnp.clip(1.0 + 0.18 * jax.random.normal(arg_keys[6], (HEAD_DIM,), jnp.float32), 0.1, 1.9),
        "output_matrix": draw_output_matrix(jax.random.fold_in(arg_keys[10], 71), 0),
        "branch_norm_gain": jnp.clip(1.0 + 0.18 * jax.random.normal(arg_keys[8], (D,), jnp.float32), 0.1, 1.9),
        "residual": noise(arg_keys[9], (TOKEN_TOTAL, D), 1.0, 6.0, ((0, 64), (1, 4))),
    }


epsilon = 1e-06

def block_update(state, queries, keys_in, values_in, running):
    length = running.shape[1]
    middle = length // 2
    anchor = running[:, middle - 1:middle, :]
    ending = running[:, -1:, :]
    causal = jnp.tril(jnp.ones((length, length), dtype=bool))
    highest = lax.Precision.HIGHEST
    inter = jnp.einsum('htd,hde->hte', queries * jnp.exp(running), state, precision=highest)
    scores = jnp.einsum('htd,hsd->hts', queries * jnp.exp(running - anchor), keys_in * jnp.exp(anchor - running), precision=highest)
    intra = jnp.einsum('hts,hse->hte', jnp.where(causal[None], scores, 0.0), values_in, precision=highest)
    new_state = state * jnp.exp(ending[:, 0, :])[:, :, None] + jnp.einsum('hsd,hse->hde', keys_in * jnp.exp(ending - running), values_in, precision=highest)
    return (new_state, inter + intra)

def head_gates(query_logits, forget_logits, value_inputs, gap):
    row_count = query_logits.shape[0]
    head_count = query_logits.shape[1] // HEAD_DIM

    def shaped(array):
        return array.astype(jnp.float32).reshape(row_count, head_count, HEAD_DIM)
    queries = jax.nn.silu(shaped(query_logits)) * HEAD_DIM ** (-0.5)
    keys_in = gap.reshape(head_count, HEAD_DIM) * jax.nn.sigmoid(-shaped(forget_logits))
    values_in = shaped(value_inputs)
    decay_factors = jnp.log1p(-keys_in)
    return (queries, keys_in, values_in, decay_factors)

def gated_norm(heads_out, output_gate_logits, head_norm_gain):
    mean_sq = lax.optimization_barrier(jnp.mean(heads_out * heads_out, axis=-1, keepdims=True))
    gates = jax.nn.silu(output_gate_logits.astype(jnp.float32).reshape(heads_out.shape))
    normed = heads_out * lax.rsqrt(mean_sq + epsilon) * head_norm_gain * gates
    return normed.reshape(heads_out.shape[0], -1).astype(jnp.bfloat16)

def reference(query_logits, forget_logits, value_inputs, output_gate_logits, forget_floor_gap, surge_log_decay, head_norm_gain, output_matrix, branch_norm_gain, residual):
    number_of_blocks = TOKEN_TOTAL // BLOCK_SPAN

    def split_into_blocks(array):
        return array.reshape(number_of_blocks, BLOCK_SPAN, array.shape[1])
    surge_values = jnp.transpose(surge_log_decay).reshape(number_of_blocks, BLOCK_SPAN, HEAD_TOTAL)

    def step_forward(state, input_tuple):
        query_tile_block, forget_gate_block, value_rows_block, output_gate_block, surge_block, residual_block = input_tuple
        queries, keys_in, values_in, decay_factors = head_gates(query_tile_block, forget_gate_block, value_rows_block, forget_floor_gap)
        decay_factors = decay_factors + surge_block[:, :, None]
        running = jnp.cumsum(jnp.transpose(decay_factors, (1, 0, 2)), axis=1)
        new_state, heads_out = block_update(state, jnp.transpose(queries, (1, 0, 2)), jnp.transpose(keys_in, (1, 0, 2)), jnp.transpose(values_in, (1, 0, 2)), running)
        mixed_rows = gated_norm(jnp.transpose(heads_out, (1, 0, 2)), output_gate_block, head_norm_gain)
        projected = lax.optimization_barrier(jnp.dot(mixed_rows, output_matrix, preferred_element_type=jnp.float32).astype(jnp.bfloat16))
        branch = projected.astype(jnp.float32)
        scale = lax.rsqrt(lax.optimization_barrier(jnp.mean(branch * branch, axis=-1, keepdims=True)) + epsilon)
        result = (residual_block.astype(jnp.float32) + branch * scale * branch_norm_gain).astype(jnp.bfloat16)
        return (new_state, result)
    starting_state = jnp.zeros((HEAD_TOTAL, HEAD_DIM, HEAD_DIM), jnp.float32)
    unused_slot, output_list = lax.scan(step_forward, starting_state, (split_into_blocks(query_logits), split_into_blocks(forget_logits), split_into_blocks(value_inputs), split_into_blocks(output_gate_logits), surge_values, split_into_blocks(residual)))
    return output_list.reshape(TOKEN_TOTAL, D)
```

```python
import jax
import jax.numpy as jnp
from jax import lax
from jax.experimental import pallas as pl
from jax.experimental.pallas import tpu as pltpu
from jax.sharding import Mesh
from jax.sharding import PartitionSpec as P

HEAD_DIM = 128
D = 4096
EPS = 1e-06
TOK = 512
HEADS = 8
CHUNK = 128
CHUNKS = TOK // CHUNK
COLS = HEADS * HEAD_DIM
NZ, NX, NC, NY = 8, 4, 2, 4
ROW = NX * NC
SP = ("z", "x", "c")
MESH = pl.DeviceIdType.MESH
F32 = jnp.float32
BF16 = jnp.bfloat16

NT = (((1,), (1,)), ((), ()))
TN = (((0,), (0,)), ((), ()))
NN = (((1,), (0,)), ((), ()))


def dot(a, b, dims=NN):
    return lax.dot_general(a, b, dims, preferred_element_type=F32)


def split2(v):
    hi = v.astype(BF16)
    return hi, (v - hi.astype(F32)).astype(BF16)


def split3(v):
    hi = v.astype(BF16)
    left = v - hi.astype(F32)
    mid = left.astype(BF16)
    return hi.astype(F32), mid.astype(F32), left - mid.astype(F32)


def log_rows(v):
    hi, mid, lo = split3(v)
    row = lax.broadcasted_iota(jnp.int32, (16, HEAD_DIM), 0)
    block = jnp.where(row == 0, hi, jnp.where(row == 1, mid, jnp.where(row == 2, lo, 0.0)))
    return block.astype(BF16)


def rows_log(block):
    return jnp.sum(block.astype(F32), axis=0, keepdims=True)


def kernel(
    q_hbm, f_hbm, v_hbm, g_hbm, w_hbm, res_hbm, gap_ref, surge_ref, hgain_ref, bgain_ref,
    out_ref,
    qb, fb, vb, gb, resb, wf, mix, ra, kt, qe, intra, gate, deltas, rows, tri, surge3,
    send1, recv1, prefix, plog, send2, recv2, send3, recv3, sq_send, sq_recv, acc,
    load_sem, s1, r1, s2, r2, s3, r3, ys, yr, yfs, yfr, wzs, wzr, wxs, wxr, wfs, wfr, wds, wdr, qs_, qr_,
):
    z, x, c, y = (lax.axis_index(n) for n in ("z", "x", "c", "y"))
    rank = x * NC + c

    def at_row(r):
        return (z, lax.div(r, NC), lax.rem(r, NC), y)

    def at_z(k):
        return (lax.rem(z + k + NZ, NZ), x, c, y)

    def at_x(k):
        return (z, lax.rem(x + k + NX, NX), c, y)

    def at_y(k):
        return (z, x, c, lax.rem(y + k + NY, NY))

    sibling = (z, x, 1 - c, y)

    def remote(src, dst, send, recv, to):
        return pltpu.make_async_remote_copy(
            src_ref=src, dst_ref=dst, send_sem=send, recv_sem=recv, device_id=to, device_id_type=MESH
        )

    started = []

    def go(*args):
        copy = remote(*args)
        copy.start()
        started.append(copy)
        return copy

    piece = (z * NX + x, c)
    loads = []
    for k, (src, dst) in enumerate(
        ((w_hbm, wf.at[piece[0], piece[1]]), (f_hbm, fb), (v_hbm, vb), (q_hbm, qb), (g_hbm, gb), (res_hbm, resb))
    ):
        copy = pltpu.make_async_copy(src, dst, load_sem.at[k])
        copy.start()
        loads.append(copy)
    barrier = pltpu.get_barrier_semaphore()
    peers = [at_row(lax.rem(rank + d, ROW)) for d in range(1, ROW)]
    peers += [at_z(d) for d in range(1, NZ)]
    peers += [at_y(d) for d in range(1, NY)]
    for peer in peers:
        pl.semaphore_signal(barrier, inc=1, device_id=peer, device_id_type=MESH)

    lane = lax.broadcasted_iota(jnp.int32, (CHUNK, 2 * CHUNK), 1)
    at = lax.broadcasted_iota(jnp.int32, (CHUNK, 2 * CHUNK), 0)
    tri[...] = jnp.where(lax.rem(lane, CHUNK) <= at, 1.0, 0.0).astype(BF16)
    hi, mid, lo = split3(surge_ref[...])
    surge3[...] = jnp.concatenate([hi, mid, lo, jnp.zeros_like(hi)], axis=0).astype(BF16)

    loads[0].wait()
    pl.semaphore_wait(barrier, len(peers))

    def w_piece(zz, xx, cc):
        return wf.at[lax.rem(zz + NZ, NZ) * NX + lax.rem(xx + NX, NX), cc]

    def w_up(step):
        return go(w_piece(z - step, x, c), w_piece(z - step, x, c), wzs.at[0, step], wzr.at[0, step], at_z(1))

    def w_down(step):
        return go(w_piece(z + step, x, c), w_piece(z + step, x, c), wzs.at[1, step], wzr.at[1, step], at_z(-1))

    w_z = [(w_up(0), w_down(0))]

    loads[1].wait()
    loads[2].wait()

    @pl.loop(0, HEADS)
    def _(h):
        cols = pl.ds(pl.multiple_of(h * HEAD_DIM, HEAD_DIM), HEAD_DIM)
        gap = gap_ref[y * HEADS + h]
        pick = lax.broadcasted_iota(jnp.int32, (32, HEAD_DIM), 0)
        pick = jnp.where(lax.rem(pick, HEADS) == h, 1.0, 0.0).astype(BF16)
        surge = dot(surge3[...], pick, TN)
        state = jnp.zeros((HEAD_DIM, HEAD_DIM), F32)
        whole = jnp.zeros((1, HEAD_DIM), F32)
        for n in range(CHUNKS):
            span = pl.ds(n * CHUNK, CHUNK)
            keys = gap / (1.0 + jnp.exp(fb[span, cols].astype(F32)))
            series = 1.0 / 8.0
            for term in range(7, 0, -1):
                series = 1.0 / term + keys * series
            decay = surge[n * CHUNK : (n + 1) * CHUNK] - keys * series
            high, low = split2(decay)
            running = dot(tri[...], jnp.concatenate([high, low], axis=0))
            anchor = running[CHUNK // 2 - 1 : CHUNK // 2]
            ending = running[CHUNK - 1 : CHUNK]
            above = running - anchor
            ra[span, cols] = above
            scaled = (keys * jnp.exp(-above)).astype(BF16)
            kt[span, cols] = scaled
            rows[h, n, 0:1] = anchor
            rows[h, n, 1:2] = ending
            delta = dot(vb[span, cols], scaled, TN) * jnp.exp(ending - anchor)
            deltas[h, n] = delta
            state = state * jnp.exp(ending) + delta
            whole = whole + ending
        send1[h, 0:HEAD_DIM] = state.astype(BF16)
        send1[h, HEAD_DIM:] = log_rows(whole)

    phase1 = []
    for d in range(1, ROW):
        t = lax.rem(rank + d, ROW)
        phase1.append(go(send1.at[t], recv1.at[d], s1.at[d], r1.at[d], at_row(t)))
    recv1[0] = send1[rank]

    w_z[0][0].wait_recv()
    w_z[0][1].wait_recv()
    w_z.append((w_up(1), w_down(1)))

    def scores_of(h):
        cols = pl.ds(pl.multiple_of(h * HEAD_DIM, HEAD_DIM), HEAD_DIM)
        gain = hgain_ref[...]
        r = lax.broadcasted_iota(jnp.int32, (CHUNK, CHUNK), 0)
        s = lax.broadcasted_iota(jnp.int32, (CHUNK, CHUNK), 1)
        for n in range(CHUNKS):
            span = pl.ds(n * CHUNK, CHUNK)
            v = qb[span, cols].astype(F32)
            queries = v / (1.0 + jnp.exp(-v)) * HEAD_DIM ** (-0.5) * jnp.exp(ra[span, cols])
            scores = dot(queries.astype(BF16), kt[span, cols], NT)
            scores = jnp.where(s <= r, scores, 0.0).astype(BF16)
            intra[span, cols] = dot(scores, vb[span, cols])
            qe[span, cols] = (queries * jnp.exp(rows[h, n, 0:1])).astype(BF16)
            v = gb[span, cols].astype(F32)
            gate[span, cols] = v / (1.0 + jnp.exp(-v)) * gain

    loads[3].wait()
    loads[4].wait()
    pl.loop(0, HEADS // 2)(scores_of)

    for copy in phase1:
        copy.wait_recv()
    total = jnp.zeros((HEAD_DIM, HEAD_DIM), F32)
    total_log = jnp.zeros((1, HEAD_DIM), F32)
    for k in range(ROW):
        slot = lax.rem(rank - k + ROW, ROW)
        prefix[k] = total
        plog[k] = total_log
        here = rows_log(recv1[slot, HEAD_DIM:])
        total = total * jnp.exp(here) + recv1[slot, 0:HEAD_DIM].astype(F32)
        total_log = total_log + here
    send2[0:HEAD_DIM] = total.astype(BF16)
    send2[HEAD_DIM:] = log_rows(total_log)

    phase2 = [go(send2, recv2.at[d], s2.at[d], r2.at[d], at_z(d)) for d in range(1, NZ)]

    w_z[1][0].wait_recv()
    w_z[1][1].wait_recv()
    w_z.append((w_up(2), w_down(2)))
    pl.loop(HEADS // 2, HEADS)(scores_of)
    w_z[2][0].wait_recv()
    w_z[2][1].wait_recv()
    w_z.append((w_up(3),))

    for copy in phase2:
        copy.wait_recv()
    carry = jnp.zeros((HEAD_DIM, HEAD_DIM), F32)
    for k in range(NZ - 1):
        slot = lax.max(lax.rem(z - k + NZ, NZ), 1)
        here = rows_log(recv2[slot, HEAD_DIM:])
        after = carry * jnp.exp(here) + recv2[slot, 0:HEAD_DIM].astype(F32)
        carry = jnp.where(k < z, after, carry)
    for d in range(ROW):
        t = lax.rem(rank + d, ROW)
        send3[d] = (prefix[t] + carry * jnp.exp(plog[t])).astype(BF16)

    phase3 = []
    for d in range(1, ROW):
        t = lax.rem(rank + d, ROW)
        phase3.append(go(send3.at[d], recv3.at[d], s3.at[d], r3.at[d], at_row(t)))
    recv3[0] = send3[0]

    w_z[3][0].wait_recv()
    offsets = (0, 1, -2, -1, 2, 3, 4, 5)
    places = [lax.rem(2 * y + o + NZ, NZ) for o in offsets]
    w_x = []
    for k, zz in enumerate(places):
        here = w_piece(zz, x, c)
        w_x.append((
            go(here, here, wxs.at[0, k], wxr.at[0, k], at_x(1)),
            go(here, here, wxs.at[1, k], wxr.at[1, k], at_x(-1)),
        ))

    for copy in phase3:
        copy.wait_recv()

    y_own = []
    for j in range(HEADS // 2):

        @pl.loop(0, 2)
        def _(i):
            h = 2 * j + i
            cols = pl.ds(pl.multiple_of(h * HEAD_DIM, HEAD_DIM), HEAD_DIM)
            half = pl.ds(pl.multiple_of(i * HEAD_DIM, HEAD_DIM), HEAD_DIM)
            state = recv3[lax.rem(rank - h + ROW, ROW)].astype(F32)
            for n in range(CHUNKS):
                span = pl.ds(n * CHUNK, CHUNK)
                heads = intra[span, cols] + dot(qe[span, cols], state.astype(BF16), NT)
                mean = jnp.sum(heads * heads, axis=1, keepdims=True) * (1.0 / HEAD_DIM)
                mix[0, j, span, half] = (heads * lax.rsqrt(mean + EPS) * gate[span, cols]).astype(BF16)
                if n < CHUNKS - 1:
                    state = state * jnp.exp(rows[h, n, 1:2]) + deltas[h, n]

        y_own.append((
            go(mix.at[0, j], mix.at[1, j], ys.at[0, j], yr.at[0, j], at_y(1)),
            go(mix.at[0, j], mix.at[2, j], ys.at[1, j], yr.at[1, j], at_y(-1)),
        ))

    w_fwd, w_core, y_fwd = [], [], []

    def w_forward(k):
        zz = places[k]
        up, down = w_x[k]
        up.wait_recv()
        down.wait_recv()
        if k % 2 == 0:
            there = w_piece(zz, x - 1, c)
            w_fwd.append(go(there, there, wfs.at[k], wfr.at[k], at_x(1)))
        else:
            there = w_piece(zz, x + 1, c)
            w_fwd.append(go(there, there, wfs.at[k], wfr.at[k], at_x(-1)))

    def w_swap(k):
        w_fwd[k].wait_recv()
        there = wf.at[pl.ds(places[k] * NX, NX), c]
        w_core.append(go(there, there, wds.at[k], wdr.at[k], sibling))

    def y_forward(j):
        up, down = y_own[j]
        up.wait_recv()
        down.wait_recv()
        if j % 2 == 0:
            y_fwd.append(go(mix.at[1, j], mix.at[3, j], yfs.at[j], yfr.at[j], at_y(1)))
        else:
            y_fwd.append(go(mix.at[2, j], mix.at[3, j], yfs.at[j], yfr.at[j], at_y(-1)))

    def multiply(slot, place, j, first=False):
        first_row = lax.rem(y + place + NY, NY) * (2 * HEADS // 2) + 2 * j

        @pl.loop(0, COLS // 256)
        def _(n):
            cols = pl.ds(pl.multiple_of(n * 256, 256), 256)
            weights = wf[pl.ds(first_row, 2), :, :, cols].reshape(256, 256)
            product = dot(mix[slot, j], weights)
            acc[:, cols] = product if first else acc[:, cols] + product

    for k in range(2):
        w_forward(k)
    for j in range(2):
        y_forward(j)
    for k in range(2, 4):
        w_forward(k)
    for j in range(2, 4):
        y_forward(j)
    for k in range(4, 8):
        w_forward(k)
    for k in range(8):
        w_swap(k)
    for k in range(2):
        w_core[k].wait_recv()
    for j in range(4):
        multiply(0, 0, j, j == 0)
    for k in range(2, 4):
        w_core[k].wait_recv()
    for j in range(4):
        multiply(1, -1, j)
    for k in range(4, 6):
        w_core[k].wait_recv()
    for j in range(4):
        multiply(2, 1, j)
    for k in range(6, 8):
        w_core[k].wait_recv()
    for j in range(4):
        y_fwd[j].wait_recv()
        multiply(3, 2, j)

    part = jnp.zeros((8, TOK), F32)
    ones = jnp.ones((8, 256), BF16)
    for n in range(COLS // 256):
        branch = acc[:, n * 256 : (n + 1) * 256].astype(BF16).astype(F32)
        high, low = split2(branch * branch)
        part = part + dot(ones, high, NT) + dot(ones, low, NT)
    sq_send[...] = part
    squares = [go(sq_send, sq_recv.at[d], qs_.at[d], qr_.at[d], at_y(d)) for d in range(1, NY)]
    for copy in squares:
        copy.wait_recv()
    for d in range(1, NY):
        part = part + sq_recv[d]
    scale = lax.rsqrt(part * (1.0 / D) + EPS)
    hi, mid, lo = split3(scale)
    parts = jnp.concatenate([hi, mid, lo, jnp.zeros_like(lo)], axis=0).astype(BF16)
    pick = lax.broadcasted_iota(jnp.int32, (32, HEAD_DIM), 0)
    pick = jnp.where(lax.rem(pick, 8) == 0, 1.0, 0.0).astype(BF16)
    column = dot(parts, pick, TN)
    loads[5].wait()

    for h in range(HEADS):
        cols = slice(h * HEAD_DIM, (h + 1) * HEAD_DIM)
        branch = acc[:, cols].astype(BF16).astype(F32)
        out_ref[:, cols] = (
            resb[:, cols].astype(F32) + branch * column * bgain_ref[y * HEADS + h]
        ).astype(BF16)

    for copy in started:
        copy.wait_send()


def per_device(q, f, v, g, gap, surge, hgain, w, bgain, res):
    any_ = pl.BlockSpec(memory_space=pl.ANY)
    vmem = pl.BlockSpec(memory_space=pltpu.VMEM)
    dma = pltpu.SemaphoreType.DMA
    block = (TOK, COLS)
    square = (HEAD_DIM, HEAD_DIM)
    message = (HEAD_DIM + 16, HEAD_DIM)
    scratch = [
        pltpu.VMEM(block, BF16),
        pltpu.VMEM(block, BF16),
        pltpu.VMEM(block, BF16),
        pltpu.VMEM(block, BF16),
        pltpu.VMEM(block, BF16),
        pltpu.VMEM((NZ * NX, NC, 64, COLS), BF16),
        pltpu.VMEM((NY, HEADS // 2, TOK, 256), BF16),
        pltpu.VMEM(block, F32),
        pltpu.VMEM(block, BF16),
        pltpu.VMEM(block, BF16),
        pltpu.VMEM(block, F32),
        pltpu.VMEM(block, F32),
        pltpu.VMEM((HEADS, CHUNKS) + square, F32),
        pltpu.VMEM((HEADS, CHUNKS, 8, HEAD_DIM), F32),
        pltpu.VMEM((CHUNK, 2 * CHUNK), BF16),
        pltpu.VMEM((32, TOK), BF16),
        pltpu.VMEM((ROW,) + message, BF16),
        pltpu.VMEM((ROW,) + message, BF16),
        pltpu.VMEM((ROW,) + square, F32),
        pltpu.VMEM((ROW, 1, HEAD_DIM), F32),
        pltpu.VMEM(message, BF16),
        pltpu.VMEM((NZ,) + message, BF16),
        pltpu.VMEM((ROW,) + square, BF16),
        pltpu.VMEM((ROW,) + square, BF16),
        pltpu.VMEM((8, TOK), F32),
        pltpu.VMEM((NY, 8, TOK), F32),
        pltpu.VMEM(block, F32),
        dma((6,)),
        dma((ROW,)), dma((ROW,)), dma((NZ,)), dma((NZ,)), dma((ROW,)), dma((ROW,)),
        dma((2, 4)), dma((2, 4)), dma((4,)), dma((4,)),
        dma((2, 4)), dma((2, 4)), dma((2, 8)), dma((2, 8)), dma((8,)), dma((8,)), dma((8,)), dma((8,)),
        dma((NY,)), dma((NY,)),
    ]
    return pl.pallas_call(
        kernel,
        out_shape=jax.ShapeDtypeStruct(block, BF16),
        in_specs=[any_] * 6 + [vmem] * 4,
        out_specs=vmem,
        scratch_shapes=scratch,
        compiler_params=pltpu.CompilerParams(
            collective_id=0, has_side_effects=True, vmem_limit_bytes=62 * 1024 * 1024
        ),
    )(
        q, f, v, g, w, res,
        gap.reshape(NY * HEADS, 1, HEAD_DIM), surge, hgain.reshape(1, HEAD_DIM),
        bgain.reshape(NY * HEADS, 1, HEAD_DIM),
    )


def solution(mesh):
    torus = Mesh(mesh.devices.reshape(NZ, NX, NC, NY), ("z", "x", "c", "y"))
    cut = P(SP, "y")
    in_specs = (cut, cut, cut, cut, P(), P("y", SP), P(), cut, P(), cut)
    return jax.shard_map(per_device, mesh=torus, in_specs=in_specs, out_specs=cut, check_vma=False)
```

```python
import jax
import jax.numpy as jnp
from jax import lax
from jax.experimental import pallas as pl
from jax.experimental.pallas import tpu as pltpu
from jax.sharding import Mesh
from jax.sharding import PartitionSpec as P

HEAD_DIM = 128
D = 4096
EPS = 1e-06
LOG2E = 1.4426950408889634
TOK = 512
HEADS = 8
CHUNK = 128
CHUNKS = TOK // CHUNK
COLS = HEADS * HEAD_DIM
NZ, NX, NC, NY = 8, 4, 2, 4
ROW = NX * NC
GROUPS = 4
GROUP_HEADS = HEADS // GROUPS
SPLIT = ROW // GROUP_HEADS
PART = HEAD_DIM // SPLIT
PAIR = 2 * HEAD_DIM
VMEM_LIMIT = 65_980_000
SP = ("z", "x", "c")
MESH = pl.DeviceIdType.MESH
F32 = jnp.float32
BF16 = jnp.bfloat16

NT = (((1,), (1,)), ((), ()))
TN = (((0,), (0,)), ((), ()))
NN = (((1,), (0,)), ((), ()))

LOG_SERIES = (1.442695046784621, 0.7213445806373628, 0.48113117086413326, 0.3542908416742433, 0.3582091924805078)


def dot(a, b, dims=NN):
    return lax.dot_general(a, b, dims, preferred_element_type=F32)


def split2(v):
    hi = v.astype(BF16)
    return hi, (v - hi.astype(F32)).astype(BF16)


def split3(v):
    hi = v.astype(BF16).astype(F32)
    left = v - hi
    mid = left.astype(BF16).astype(F32)
    return hi, mid, left - mid


def log_rows(v):
    hi, mid, lo = split3(v)
    row = lax.broadcasted_iota(jnp.int32, (16, HEAD_DIM), 0)
    block = jnp.where(row == 0, hi, jnp.where(row == 1, mid, jnp.where(row == 2, lo, 0.0)))
    return block.astype(BF16)


def rows_log(block):
    return jnp.sum(block.astype(F32), axis=0, keepdims=True)


def kernel(
    q_hbm, f_hbm, v_hbm, g_hbm, w_hbm, res_hbm, gap_ref, surge_ref, hgain_ref, bgain_ref,
    out_ref,
    qb, fb, vb, gb, branch_buf, resb, wf, mix, ra, kt, qe, intra, gate, deltas, rows, tri, surge3,
    send1, recv1, prefix, plog, send2, recv2, send3, recv3, sq_send, sq_recv, acc,
    load_sem, s1, r1, s2, r2, s3, r3, ys, yr, yfs, yfr,
    azs, azr, bxs, bxr, bfs, bfr, axs, axr, afs, afr, bzs, bzr, wds, wdr, qs_, qr_,
):
    z, x, c, y = (lax.axis_index(n) for n in ("z", "x", "c", "y"))
    rank = x * NC + c

    def at_row(r):
        return (z, lax.div(r, NC), lax.rem(r, NC), y)

    def wrap_z(k):
        return lax.rem(z + k + NZ, NZ)

    def wrap_x(k):
        return lax.rem(x + k + NX, NX)

    def at_z(k):
        return (wrap_z(k), x, c, y)

    def at_x(k):
        return (z, wrap_x(k), c, y)

    def at_y(k):
        return (z, x, c, lax.rem(y + k + NY, NY))

    sibling = (z, x, 1 - c, y)
    started = []

    def go(src, dst, send, recv, to):
        copy = pltpu.make_async_remote_copy(
            src_ref=src, dst_ref=dst, send_sem=send, recv_sem=recv, device_id=to, device_id_type=MESH
        )
        copy.start()
        started.append(copy)
        return copy

    EARLY, LATE = pl.ds(0, COLS // 2), pl.ds(COLS // 2, COLS // 2)
    loads = []
    for k, (src, dst) in enumerate(
        (
            (f_hbm.at[:, EARLY], fb.at[:, EARLY]), (v_hbm.at[:, EARLY], vb.at[:, EARLY]), (w_hbm, wf.at[z, x, c]),
            (f_hbm.at[:, LATE], fb.at[:, LATE]), (v_hbm.at[:, LATE], vb.at[:, LATE]), (q_hbm, qb), (g_hbm, gb),
            (res_hbm, resb),
        )
    ):
        copy = pltpu.make_async_copy(src, dst, load_sem.at[k])
        copy.start()
        loads.append(copy)
    load_f, load_v, load_w, *loads_late, load_q, load_g, load_res = loads
    barrier = pltpu.get_barrier_semaphore()
    peers = [at_row(lax.rem(rank + d, ROW)) for d in range(1, ROW)]
    peers += [at_z(d) for d in range(1, NZ)]
    peers += [at_y(d) for d in range(1, NY)]
    for peer in peers:
        pl.semaphore_signal(barrier, inc=1, device_id=peer, device_id_type=MESH)

    lane = lax.broadcasted_iota(jnp.int32, (CHUNK, 2 * CHUNK), 1)
    at = lax.broadcasted_iota(jnp.int32, (CHUNK, 2 * CHUNK), 0)
    tri[...] = jnp.where(lax.rem(lane, CHUNK) <= at, 1.0, 0.0).astype(BF16)
    hi, mid, lo = split3(surge_ref[...] * LOG2E)
    surge3[...] = jnp.concatenate([hi, mid, lo, jnp.zeros_like(hi)], axis=0).astype(BF16)
    load_f.wait()
    load_v.wait()

    def states_of(p):
        cols = pl.ds(pl.multiple_of(p * PAIR, PAIR), PAIR)
        gap = gap_ref[y * (HEADS // 2) + p] * 0.5
        pick = lax.broadcasted_iota(jnp.int32, (32, PAIR), 0)
        head = 2 * p + lax.div(lax.broadcasted_iota(jnp.int32, (32, PAIR), 1), HEAD_DIM)
        pick = jnp.where(lax.rem(pick, HEADS) == head, 1.0, 0.0).astype(BF16)
        surge = dot(surge3[...], pick, TN)
        state = [jnp.zeros((HEAD_DIM, HEAD_DIM), F32)] * 2
        whole = jnp.zeros((1, PAIR), F32)
        for n in range(CHUNKS):
            span = pl.ds(n * CHUNK, CHUNK)
            keys = gap - gap * jnp.tanh(fb[span, cols].astype(F32) * 0.5)
            series = LOG_SERIES[-1]
            for term in LOG_SERIES[-2::-1]:
                series = term + keys * series
            decay = surge[n * CHUNK : (n + 1) * CHUNK] - keys * series
            high, low = split2(decay)
            running = dot(tri[...], jnp.concatenate([high, low], axis=0))
            anchor = running[CHUNK // 2 - 1 : CHUNK // 2]
            ending = running[CHUNK - 1 : CHUNK]
            above = running - anchor
            ra[span, cols] = above
            scaled = (keys * jnp.exp2(-above)).astype(BF16)
            kt[span, cols] = scaled
            shrink = jnp.exp2(ending)
            tail = jnp.exp2(ending - anchor)
            rows[p, n, 0:1] = jnp.exp2(anchor)
            rows[p, n, 1:2] = shrink
            values = vb[span, cols]
            for i in range(2):
                half = slice(i * HEAD_DIM, (i + 1) * HEAD_DIM)
                delta = dot(values[:, half], scaled[:, half], TN) * tail[:, half]
                deltas[2 * p + i, n] = delta
                state[i] = state[i] * shrink[:, half] + delta
            whole = whole + ending
        for i in range(2):
            block = state[i].astype(BF16)
            logs = log_rows(whole[:, i * HEAD_DIM : (i + 1) * HEAD_DIM])
            for e in range(SPLIT):
                send1[p, SPLIT * i + e, 0:PART] = block[e * PART : (e + 1) * PART]
                send1[p, SPLIT * i + e, PART:] = logs

    def send_states(g):
        copies = []
        for d in range(1, ROW):
            t = lax.rem(rank + d, ROW)
            copies.append(go(send1.at[g, t], recv1.at[g, d], s1.at[g, d], r1.at[g, d], at_row(t)))
        recv1[g, 0] = send1[g, rank]
        return copies

    def send_totals(g, arriving):
        for copy in arriving:
            copy.wait_recv()
        total = jnp.zeros((PART, HEAD_DIM), F32)
        total_log = jnp.zeros((1, HEAD_DIM), F32)
        for k in range(ROW):
            slot = lax.rem(rank - k + ROW, ROW)
            prefix[g, k] = total
            plog[g, k] = total_log
            here = rows_log(recv1[g, slot, PART:])
            total = total * jnp.exp2(here) + recv1[g, slot, 0:PART].astype(F32)
            total_log = total_log + here
        send2[g, 0:PART] = total.astype(BF16)
        send2[g, PART:] = log_rows(total_log)
        return [go(send2.at[g], recv2.at[g, d], s2.at[g, d], r2.at[g, d], at_z(d)) for d in range(1, NZ)]

    def send_carried(g, arriving):
        for copy in arriving:
            copy.wait_recv()
        carry = jnp.zeros((PART, HEAD_DIM), F32)
        for k in range(NZ - 1):
            slot = lax.max(lax.rem(z - k + NZ, NZ), 1)
            here = rows_log(recv2[g, slot, PART:])
            after = carry * jnp.exp2(here) + recv2[g, slot, 0:PART].astype(F32)
            carry = jnp.where(k < z, after, carry)
        copies = []
        for d in range(ROW):
            t = lax.rem(rank + d, ROW)
            send3[g, d] = (prefix[g, t] + carry * jnp.exp2(plog[g, t])).astype(BF16)
            if d > 0:
                copies.append(go(send3.at[g, d], recv3.at[g, d], s3.at[g, d], r3.at[g, d], at_row(t)))
        recv3[g, 0] = send3[g, 0]
        return copies

    def scores_of(p):
        gain = hgain_ref[...] * 0.5
        r = lax.broadcasted_iota(jnp.int32, (CHUNK, CHUNK), 0)
        s = lax.broadcasted_iota(jnp.int32, (CHUNK, CHUNK), 1)
        for i in range(2):
            cols = pl.ds(pl.multiple_of(p * PAIR + i * HEAD_DIM, HEAD_DIM), HEAD_DIM)
            for n in range(CHUNKS):
                span = pl.ds(n * CHUNK, CHUNK)
                v = qb[span, cols].astype(F32)
                h = v * (0.5 * HEAD_DIM ** (-0.5))
                queries = (h + h * jnp.tanh(v * 0.5)) * jnp.exp2(ra[span, cols])
                scores = dot(queries.astype(BF16), kt[span, cols], NT)
                scores = jnp.where(s <= r, scores, 0.0).astype(BF16)
                intra[span, cols] = dot(scores, vb[span, cols])
                qe[span, cols] = (queries * rows[p, n, 0:1, i * HEAD_DIM : (i + 1) * HEAD_DIM]).astype(BF16)
                v = gb[span, cols].astype(F32)
                h = v * gain
                gate[span, cols] = h + h * jnp.tanh(v * 0.5)

    y_own = []

    def finish(j):
        for i in range(2):
            h = 2 * j + i
            cols = pl.ds(h * HEAD_DIM, HEAD_DIM)
            slots = [lax.rem(rank - (SPLIT * i + e) + ROW, ROW) for e in range(SPLIT)]
            state = jnp.concatenate([recv3[j, slot].astype(F32) for slot in slots], axis=0)
            for n in range(CHUNKS):
                span = pl.ds(n * CHUNK, CHUNK)
                heads = intra[span, cols] + dot(qe[span, cols], state.astype(BF16), NT)
                mean = jnp.sum(heads * heads, axis=1, keepdims=True) * (1.0 / HEAD_DIM)
                mix[0, span, cols] = (heads * lax.rsqrt(mean + EPS) * gate[span, cols]).astype(BF16)
                if n < CHUNKS - 1:
                    state = state * rows[j, n, 1:2, i * HEAD_DIM : (i + 1) * HEAD_DIM] + deltas[h, n]
        part = pl.ds(j * PAIR, PAIR)
        y_own.append((
            go(mix.at[0, :, part], mix.at[1, :, part], ys.at[0, j], yr.at[0, j], at_y(1)),
            go(mix.at[0, :, part], mix.at[2, :, part], ys.at[1, j], yr.at[1, j], at_y(-1)),
        ))

    A, B = pl.ds(0, 32), pl.ds(32, 32)

    OFFSETS = (0, -1, 1, -2, 2, -3, 3, 4)

    def a_send(k, offset, d):
        ref = wf.at[wrap_z(offset), x, c, A]
        return go(ref, ref, azs.at[k], azr.at[k], at_z(d))

    away = 2 - 4 * c

    def a_out(k):
        ref = wf.at[wrap_z(OFFSETS[k]), x, c, A]
        return [go(ref, ref, axs.at[i, k], axr.at[i, k], at_x(d)) for i, d in enumerate((1, -1))]

    def a_forward(k):
        wait_both(a_x[k])
        d = 1 if k % 2 == 0 else -1
        ref = wf.at[wrap_z(OFFSETS[k]), wrap_x(-d), c, A]
        return go(ref, ref, afs.at[k], afr.at[k], at_x(d))

    def b_go(way, step, m):
        ref = wf.at[wrap_z(step if way else -step), pl.ds(2 * m, 2), c, B]
        return go(ref, ref, bzs.at[way, step, m], bzr.at[way, step, m], at_z(-1 if way else 1))

    def b_send(step):
        return [[b_go(way, step, m) for way in range(2)] for m in range(2)]

    def b_next(step):
        b_ring.append([])
        for m in range(2):
            wait_both(b_ring[step - 1][m])
            b_ring[step].append([b_go(way, step, m) for way in range(2) if step < 3 or way == m])

    def wait_both(copies):
        for copy in copies:
            copy.wait_recv()

    swaps = []

    def swap(ref):
        k = len(swaps)
        swaps.append(go(ref, ref, wds.at[k], wdr.at[k], sibling))

    pl.loop(0, 2)(states_of)
    pl.semaphore_wait(barrier, len(peers))
    arriving1 = [send_states(0), send_states(1)]
    load_w.wait()
    a_z = [a_send(0, 0, 1), a_send(1, 0, -1), a_send(2, 0, 2), a_send(3, 0, -2)]
    own_b = wf.at[z, x, c, B]
    b_x = (go(own_b, own_b, bxs.at[0], bxr.at[0], at_x(1)), go(own_b, own_b, bxs.at[1], bxr.at[1], at_x(-1)))
    loads_late[0].wait()
    loads_late[1].wait()
    states_of(2)
    arriving1.append(send_states(2))
    states_of(3)
    arriving1.append(send_states(3))
    load_q.wait()
    load_g.wait()
    scores_of(0)
    arriving2 = [send_totals(0, arriving1[0])]
    arriving2.append(send_totals(1, arriving1[1]))
    scores_of(1)
    arriving2.append(send_totals(2, arriving1[2]))
    arriving2.append(send_totals(3, arriving1[3]))
    scores_of(2)
    arriving3 = [send_carried(0, arriving2[0])]
    arriving3.append(send_carried(1, arriving2[1]))
    wait_both(b_x)
    ref = wf.at[z, wrap_x(-1), c, pl.ds(32, 16)]
    b_f = [go(ref, ref, bfs.at[0], bfr.at[0], at_x(1))]
    ref = wf.at[z, wrap_x(1), c, pl.ds(48, 16)]
    b_f.append(go(ref, ref, bfs.at[1], bfr.at[1], at_x(-1)))
    wait_both(a_z[0:4])
    a_z += [a_send(4, -2, 1), a_send(5, 2, -1), a_send(6, -away, away)]
    a_x = [a_out(k) for k in range(3)]
    scores_of(3)
    wait_both(arriving3[0])
    finish(0)
    wait_both(b_f)
    b_ring = [b_send(0)]
    wait_both(arriving3[1])
    finish(1)
    arriving3.append(send_carried(2, arriving2[2]))
    arriving3.append(send_carried(3, arriving2[3]))
    a_x += [a_out(k) for k in range(3, 5)]
    a_f = [a_forward(k) for k in range(3)]
    wait_both(arriving3[2])
    finish(2)
    wait_both(arriving3[3])
    finish(3)

    wait_both(a_z[4:7])
    a_x += [a_out(k) for k in range(5, 8)]
    b_next(1)
    for k in (0, -1, 1):
        swap(wf.at[wrap_z(k), :, c, B])
    a_f += [a_forward(k) for k in range(3, 5)]
    b_next(2)
    for k in (-2, 2):
        swap(wf.at[wrap_z(k), :, c, B])
    a_f += [a_forward(k) for k in range(5, 8)]
    y_fwd = []

    HALVES = (pl.ds(0, TOK // 2), pl.ds(TOK // 2, TOK // 2))

    def y_forward(j):
        wait_both(y_own[j])
        part = pl.ds(j * PAIR, PAIR)
        d = 1 if j % 2 == 0 else -1
        source = 1 if d == 1 else 2
        y_fwd.append([
            go(mix.at[source, half, part], mix.at[3, half, part], yfs.at[j, m], yfr.at[j, m], at_y(d))
            for m, half in enumerate(HALVES)
        ])

    y_forward(0)
    y_forward(1)
    b_next(3)
    for k in (-3, 3):
        swap(wf.at[wrap_z(k), :, c, B])
    wait_both(a_f)
    for m in range(2):
        swap(wf.at[pl.ds(4 * m, 4), :, c, A])
    y_forward(2)
    y_forward(3)
    for m in range(2):
        wait_both(b_ring[3][m])
    swap(wf.at[wrap_z(4), :, c, B])
    wait_both(swaps)

    def multiply(slot, place, m=None, rows_=pl.ds(0, TOK)):
        first = 2 * lax.rem(y + place + NY, NY)
        depth = COLS if m is None else COLS // 2
        left = pl.ds(0 if m is None else m * depth, depth)

        @pl.loop(0, COLS // 256)
        def _(n):
            cols = pl.ds(pl.multiple_of(n * 256, 256), 256)
            if m is None:
                weights = wf[pl.ds(first, 2), :, :, :, cols].reshape(depth, 256)
            else:
                weights = wf[first + m, :, :, :, cols].reshape(depth, 256)
            product = dot(mix[slot, rows_, left], weights)
            acc[rows_, cols] = product if slot == 0 else acc[rows_, cols] + product

    for slot, place in ((0, 0), (1, -1), (2, 1)):
        multiply(slot, place)
    wait_both(y_fwd[0] + y_fwd[1])
    multiply(3, 2, 0)

    load_res.wait()

    def squares_of(m):
        rows_ = HALVES[m]
        wait_both((y_fwd[2][m], y_fwd[3][m]))
        multiply(3, 2, 1, rows_)
        part = jnp.zeros((8, TOK // 2), F32)
        ones = jnp.ones((8, 256), BF16)
        for n in range(COLS // 256):
            cols = slice(n * 256, (n + 1) * 256)
            branch = acc[rows_, cols].astype(BF16)
            branch_buf[rows_, cols] = branch
            branch = branch.astype(F32)
            high, low = split2(branch * branch)
            part = part + dot(ones, high, NT) + dot(ones, low, NT)
        sq_send[m] = part
        return [go(sq_send.at[m], sq_recv.at[m, d], qs_.at[m, d], qr_.at[m, d], at_y(d)) for d in range(1, NY)]

    def write(m, squares):
        rows_ = HALVES[m]
        wait_both(squares)
        part = sq_send[m]
        for d in range(1, NY):
            part = part + sq_recv[m, d]
        scale = lax.rsqrt(part * (1.0 / D) + EPS)
        hi, mid, lo = split3(scale)
        parts = jnp.concatenate([hi, mid, lo, jnp.zeros_like(lo)], axis=0).astype(BF16)
        pick = lax.broadcasted_iota(jnp.int32, (32, HEAD_DIM), 0)
        pick = jnp.where(lax.rem(pick, 8) == 0, 1.0, 0.0).astype(BF16)
        column = dot(parts, pick, TN)
        for h in range(HEADS):
            cols = slice(h * HEAD_DIM, (h + 1) * HEAD_DIM)
            out_ref[rows_, cols] = (
                resb[rows_, cols].astype(F32) + branch_buf[rows_, cols].astype(F32) * column * bgain_ref[y * HEADS + h]
            ).astype(BF16)

    squares = [squares_of(0)]
    squares.append(squares_of(1))
    write(0, squares[0])
    write(1, squares[1])
    for copy in started:
        copy.wait_send()


def per_device(q, f, v, g, gap, surge, hgain, w, bgain, res):
    any_ = pl.BlockSpec(memory_space=pltpu.HBM)
    vmem = pl.BlockSpec(memory_space=pltpu.VMEM)
    dma = pltpu.SemaphoreType.DMA
    block = (TOK, COLS)
    state = (PART, HEAD_DIM)
    message = (PART + 16, HEAD_DIM)
    scratch = [
        pltpu.VMEM(block, BF16),
        pltpu.VMEM(block, BF16),
        pltpu.VMEM(block, BF16),
        pltpu.VMEM(block, BF16),
        pltpu.VMEM(block, BF16),
        pltpu.VMEM(block, BF16),
        pltpu.VMEM((NZ, NX, NC, 64, COLS), BF16),
        pltpu.VMEM((NY,) + block, BF16),
        pltpu.VMEM(block, F32),
        pltpu.VMEM(block, BF16),
        pltpu.VMEM(block, BF16),
        pltpu.VMEM(block, F32),
        pltpu.VMEM(block, F32),
        pltpu.VMEM((HEADS, CHUNKS, HEAD_DIM, HEAD_DIM), F32),
        pltpu.VMEM((HEADS // 2, CHUNKS, 8, PAIR), F32),
        pltpu.VMEM((CHUNK, 2 * CHUNK), BF16),
        pltpu.VMEM((32, TOK), BF16),
        pltpu.VMEM((GROUPS, ROW) + message, BF16),
        pltpu.VMEM((GROUPS, ROW) + message, BF16),
        pltpu.VMEM((GROUPS, ROW) + state, F32),
        pltpu.VMEM((GROUPS, ROW, 1, HEAD_DIM), F32),
        pltpu.VMEM((GROUPS,) + message, BF16),
        pltpu.VMEM((GROUPS, NZ) + message, BF16),
        pltpu.VMEM((GROUPS, ROW) + state, BF16),
        pltpu.VMEM((GROUPS, ROW) + state, BF16),
        pltpu.VMEM((2, 8, TOK // 2), F32),
        pltpu.VMEM((2, NY, 8, TOK // 2), F32),
        pltpu.VMEM(block, F32),
        dma((8,)),
        dma((GROUPS, ROW)), dma((GROUPS, ROW)), dma((GROUPS, NZ)), dma((GROUPS, NZ)),
        dma((GROUPS, ROW)), dma((GROUPS, ROW)),
        dma((2, 4)), dma((2, 4)), dma((4, 2)), dma((4, 2)),
        dma((7,)), dma((7,)), dma((2,)), dma((2,)), dma((2,)), dma((2,)),
        dma((2, 8)), dma((2, 8)), dma((8,)), dma((8,)), dma((2, 4, 2)), dma((2, 4, 2)), dma((10,)), dma((10,)),
        dma((2, NY)), dma((2, NY)),
    ]
    return pl.pallas_call(
        kernel,
        out_shape=pltpu.VMEM(block, BF16),
        in_specs=[any_] * 6 + [vmem] * 4,
        out_specs=vmem,
        scratch_shapes=scratch,
        compiler_params=pltpu.CompilerParams(
            collective_id=0, has_side_effects=True, vmem_limit_bytes=VMEM_LIMIT
        ),
    )(
        q, f, v, g, w, res,
        gap.reshape(NY * HEADS // 2, 1, PAIR), surge, hgain.reshape(1, HEAD_DIM),
        bgain.reshape(NY * HEADS, 1, HEAD_DIM),
    )


def solution(mesh):
    torus = Mesh(mesh.devices.reshape(NZ, NX, NC, NY), ("z", "x", "c", "y"))
    cut = P(SP, "y")
    in_specs = (cut, cut, cut, cut, P(), P("y", SP), P(), cut, P(), cut)
    return jax.shard_map(per_device, mesh=torus, in_specs=in_specs, out_specs=cut, check_vma=False)
```

```python
import jax
import jax.numpy as jnp
from jax import lax
from jax.experimental import pallas as pl
from jax.experimental.pallas import tpu as pltpu
from jax.sharding import Mesh
from jax.sharding import PartitionSpec as P

HEAD_DIM = 128
D = 4096
EPS = 1e-06
LOG2E = 1.4426950408889634
TOK = 512
HEADS = 8
CHUNK = 128
CHUNKS = TOK // CHUNK
COLS = HEADS * HEAD_DIM
NZ, NX, NC, NY = 8, 4, 2, 4
ROW = NX * NC
GROUPS = 4
GROUP_HEADS = HEADS // GROUPS
SPLIT = ROW // GROUP_HEADS
PART = HEAD_DIM // SPLIT
PAIR = 2 * HEAD_DIM
VMEM_LIMIT = 65_980_000
SP = ("z", "x", "c")
MESH = pl.DeviceIdType.MESH
F32 = jnp.float32
BF16 = jnp.bfloat16

NT = (((1,), (1,)), ((), ()))
TN = (((0,), (0,)), ((), ()))
NN = (((1,), (0,)), ((), ()))

LOG_SERIES = (1.442695046784621, 0.7213445806373628, 0.48113117086413326, 0.3542908416742433, 0.3582091924805078)


def dot(a, b, dims=NN):
    return lax.dot_general(a, b, dims, preferred_element_type=F32)


def split2(v):
    hi = v.astype(BF16)
    return hi, (v - hi.astype(F32)).astype(BF16)


def split3(v):
    hi = v.astype(BF16).astype(F32)
    left = v - hi
    mid = left.astype(BF16).astype(F32)
    return hi, mid, left - mid


def log_rows(v):
    hi, mid, lo = split3(v)
    row = lax.broadcasted_iota(jnp.int32, (16, HEAD_DIM), 0)
    block = jnp.where(row == 0, hi, jnp.where(row == 1, mid, jnp.where(row == 2, lo, 0.0)))
    return block.astype(BF16)


def rows_log(block):
    return jnp.sum(block.astype(F32), axis=0, keepdims=True)


def kernel(
    q_hbm, f_hbm, v_hbm, g_hbm, w_hbm, res_hbm, gap_hbm, surge_hbm, hgain_hbm, bgain_hbm,
    out_ref,
    qb, fb, vb, gb, branch_buf, resb, gap_ref, surge_ref, hgain_ref, bgain_ref, wf, mix,
    ra, kt, qe, intra, gate, deltas, rows, tri, surge3,
    send1, recv1, prefix, plog, send2, recv2, send3, recv3, sq_send, sq_recv, acc,
    load_sem, sent, r1, r2, r3, yr, yfr, ar, br, wdr, qr_,
):
    z, x, c, y = (lax.axis_index(n) for n in ("z", "x", "c", "y"))
    rank = x * NC + c

    def at_row(r):
        return (z, lax.div(r, NC), lax.rem(r, NC), y)

    def wrap_z(k):
        return lax.rem(z + k + NZ, NZ)

    def wrap_x(k):
        return lax.rem(x + k + NX, NX)

    def at_z(k):
        return (wrap_z(k), x, c, y)

    def at_x(k):
        return (z, wrap_x(k), c, y)

    def at_y(k):
        return (z, x, c, lax.rem(y + k + NY, NY))

    sibling = (z, x, 1 - c, y)

    def done(sem, view):
        pltpu.make_async_copy(view, view, sem).wait()

    PHASE1, PHASE2, PHASE3, OVER_Y, A_Z, A_X, B_X, B_Z, CORES, SQUARES = (sent.at[k] for k in range(10))

    def go(src, dst, send, recv, to):
        copy = pltpu.make_async_remote_copy(
            src_ref=src, dst_ref=dst, send_sem=send, recv_sem=recv, device_id=to, device_id_type=MESH
        )
        copy.start()

    EARLY, LATE = pl.ds(0, COLS // 2), pl.ds(COLS // 2, COLS // 2)
    barrier = pltpu.get_barrier_semaphore()
    peers = [at_row(lax.rem(rank + d, ROW)) for d in range(1, ROW)]
    peers += [at_z(d) for d in range(1, NZ)]
    peers += [at_y(d) for d in range(1, NY)]
    for peer in peers:
        pl.semaphore_signal(barrier, inc=1, device_id=peer, device_id_type=MESH)

    def load(k, *pairs):
        for src, dst in pairs:
            pltpu.make_async_copy(src, dst, load_sem.at[k]).start()

    load(0, (f_hbm.at[:, EARLY], fb.at[:, EARLY]), (v_hbm.at[:, EARLY], vb.at[:, EARLY]))
    load(1, (surge_hbm, surge_ref))
    load(2, (gap_hbm, gap_ref))
    load(3, (w_hbm, wf.at[z, x, c]))
    load(4, (f_hbm.at[:, LATE], fb.at[:, LATE]), (v_hbm.at[:, LATE], vb.at[:, LATE]))
    load(5, (q_hbm, qb), (g_hbm, gb))
    load(6, (hgain_hbm, hgain_ref))
    load(7, (bgain_hbm, bgain_ref))
    load(8, (res_hbm, resb))
    lane = lax.broadcasted_iota(jnp.int32, (CHUNK, 2 * CHUNK), 1)
    at = lax.broadcasted_iota(jnp.int32, (CHUNK, 2 * CHUNK), 0)
    tri[...] = jnp.where(lax.rem(lane, CHUNK) <= at, 1.0, 0.0).astype(BF16)
    done(load_sem.at[1], surge_ref)
    hi, mid, lo = split3(surge_ref[...] * LOG2E)
    surge3[...] = jnp.concatenate([hi, mid, lo, jnp.zeros_like(hi)], axis=0).astype(BF16)
    done(load_sem.at[2], gap_ref)
    done(load_sem.at[0], fb)

    def states_of(p):
        cols = pl.ds(pl.multiple_of(p * PAIR, PAIR), PAIR)
        gap = gap_ref[y * (HEADS // 2) + p] * 0.5
        pick = lax.broadcasted_iota(jnp.int32, (32, PAIR), 0)
        head = 2 * p + lax.div(lax.broadcasted_iota(jnp.int32, (32, PAIR), 1), HEAD_DIM)
        pick = jnp.where(lax.rem(pick, HEADS) == head, 1.0, 0.0).astype(BF16)
        surge = dot(surge3[...], pick, TN)
        state = [jnp.zeros((HEAD_DIM, HEAD_DIM), F32)] * 2
        whole = jnp.zeros((1, PAIR), F32)
        for n in range(CHUNKS):
            span = pl.ds(n * CHUNK, CHUNK)
            keys = gap - gap * jnp.tanh(fb[span, cols].astype(F32) * 0.5)
            series = LOG_SERIES[-1]
            for term in LOG_SERIES[-2::-1]:
                series = term + keys * series
            decay = surge[n * CHUNK : (n + 1) * CHUNK] - keys * series
            high, low = split2(decay)
            running = dot(tri[...], jnp.concatenate([high, low], axis=0))
            anchor = running[CHUNK // 2 - 1 : CHUNK // 2]
            ending = running[CHUNK - 1 : CHUNK]
            above = running - anchor
            ra[span, cols] = above
            scaled = (keys * jnp.exp2(-above)).astype(BF16)
            kt[span, cols] = scaled
            shrink = jnp.exp2(ending)
            tail = jnp.exp2(ending - anchor)
            rows[p, n, 0:1] = jnp.exp2(anchor)
            rows[p, n, 1:2] = shrink
            values = vb[span, cols]
            for i in range(2):
                half = slice(i * HEAD_DIM, (i + 1) * HEAD_DIM)
                delta = dot(values[:, half], scaled[:, half], TN) * tail[:, half]
                deltas[2 * p + i, n] = delta
                state[i] = state[i] * shrink[:, half] + delta
            whole = whole + ending
        for i in range(2):
            block = state[i].astype(BF16)
            logs = log_rows(whole[:, i * HEAD_DIM : (i + 1) * HEAD_DIM])
            for e in range(SPLIT):
                send1[p, SPLIT * i + e, 0:PART] = block[e * PART : (e + 1) * PART]
                send1[p, SPLIT * i + e, PART:] = logs

    def send_states(g):
        for d in range(1, ROW):
            t = lax.rem(rank + d, ROW)
            go(send1.at[g, t], recv1.at[g, d], PHASE1, r1.at[g], at_row(t))
        recv1[g, 0] = send1[g, rank]

    def send_totals(g):
        done(r1.at[g], recv1.at[g, pl.ds(1, ROW - 1)])
        total = jnp.zeros((PART, HEAD_DIM), F32)
        total_log = jnp.zeros((1, HEAD_DIM), F32)
        for k in range(ROW):
            slot = lax.rem(rank - k + ROW, ROW)
            prefix[g, k] = total
            plog[g, k] = total_log
            here = rows_log(recv1[g, slot, PART:])
            total = total * jnp.exp2(here) + recv1[g, slot, 0:PART].astype(F32)
            total_log = total_log + here
        send2[g, 0:PART] = total.astype(BF16)
        send2[g, PART:] = log_rows(total_log)
        for d in range(1, NZ):
            go(send2.at[g], recv2.at[g, d], PHASE2, r2.at[g], at_z(d))

    def send_carried(g):
        done(r2.at[g], recv2.at[g, pl.ds(1, NZ - 1)])
        carry = jnp.zeros((PART, HEAD_DIM), F32)
        for k in range(NZ - 1):
            slot = lax.max(lax.rem(z - k + NZ, NZ), 1)
            here = rows_log(recv2[g, slot, PART:])
            after = carry * jnp.exp2(here) + recv2[g, slot, 0:PART].astype(F32)
            carry = jnp.where(k < z, after, carry)
        for d in range(ROW):
            t = lax.rem(rank + d, ROW)
            send3[g, d] = (prefix[g, t] + carry * jnp.exp2(plog[g, t])).astype(BF16)
            if d > 0:
                go(send3.at[g, d], recv3.at[g, d], PHASE3, r3.at[g], at_row(t))
        recv3[g, 0] = send3[g, 0]

    def scores_of(p):
        gain = hgain_ref[...] * 0.5
        r = lax.broadcasted_iota(jnp.int32, (CHUNK, CHUNK), 0)
        s = lax.broadcasted_iota(jnp.int32, (CHUNK, CHUNK), 1)
        for i in range(2):
            cols = pl.ds(pl.multiple_of(p * PAIR + i * HEAD_DIM, HEAD_DIM), HEAD_DIM)
            for n in range(CHUNKS):
                span = pl.ds(n * CHUNK, CHUNK)
                v = qb[span, cols].astype(F32)
                h = v * (0.5 * HEAD_DIM ** (-0.5))
                queries = (h + h * jnp.tanh(v * 0.5)) * jnp.exp2(ra[span, cols])
                scores = dot(queries.astype(BF16), kt[span, cols], NT)
                scores = jnp.where(s <= r, scores, 0.0).astype(BF16)
                intra[span, cols] = dot(scores, vb[span, cols])
                qe[span, cols] = (queries * rows[p, n, 0:1, i * HEAD_DIM : (i + 1) * HEAD_DIM]).astype(BF16)
                v = gb[span, cols].astype(F32)
                h = v * gain
                gate[span, cols] = h + h * jnp.tanh(v * 0.5)

    def finish(j):
        done(r3.at[j], recv3.at[j, pl.ds(1, ROW - 1)])
        for i in range(2):
            h = 2 * j + i
            cols = pl.ds(h * HEAD_DIM, HEAD_DIM)
            slots = [lax.rem(rank - (SPLIT * i + e) + ROW, ROW) for e in range(SPLIT)]
            state = jnp.concatenate([recv3[j, slot].astype(F32) for slot in slots], axis=0)
            for n in range(CHUNKS):
                span = pl.ds(n * CHUNK, CHUNK)
                heads = intra[span, cols] + dot(qe[span, cols], state.astype(BF16), NT)
                mean = jnp.sum(heads * heads, axis=1, keepdims=True) * (1.0 / HEAD_DIM)
                mix[0, span, cols] = (heads * lax.rsqrt(mean + EPS) * gate[span, cols]).astype(BF16)
                if n < CHUNKS - 1:
                    state = state * rows[j, n, 1:2, i * HEAD_DIM : (i + 1) * HEAD_DIM] + deltas[h, n]
        part = pl.ds(j * PAIR, PAIR)
        go(mix.at[0, :, part], mix.at[1, :, part], OVER_Y, yr.at[j], at_y(1))
        go(mix.at[0, :, part], mix.at[2, :, part], OVER_Y, yr.at[j], at_y(-1))

    A, B = pl.ds(0, 32), pl.ds(32, 32)

    OFFSETS = (0, -1, 1, -2, 2, -3, 3, 4)
    BATCH = (0, 0, 0, 1, 1, 2, 2, 2)
    away = 2 - 4 * c

    def a_send(k, offset, d):
        ref = wf.at[wrap_z(offset), x, c, A]
        go(ref, ref, A_Z, ar.at[k], at_z(d))

    def a_out(k):
        ref = wf.at[wrap_z(OFFSETS[k]), x, c, A]
        for d in (1, -1):
            go(ref, ref, A_X, ar.at[2 + BATCH[k]], at_x(d))

    def a_forward(batch):
        ks = [k for k in range(NZ) if BATCH[k] == batch]
        done(ar.at[2 + batch], wf.at[pl.ds(0, len(ks)), pl.ds(0, 2), 0, A])
        for k in ks:
            d = 1 if k % 2 == 0 else -1
            ref = wf.at[wrap_z(OFFSETS[k]), wrap_x(-d), c, A]
            go(ref, ref, A_X, ar.at[5], at_x(d))

    def b_go(way, step, m):
        ref = wf.at[wrap_z(step if way else -step), pl.ds(2 * m, 2), c, B]
        go(ref, ref, B_Z, br.at[2 * step + m if step < 3 else 6], at_z(-1 if way else 1))

    def b_send(step):
        for m in range(2):
            if step > 0:
                done(br.at[2 * step - 2 + m], wf.at[pl.ds(0, 2), pl.ds(0, 2), 0, B])
            for way in range(2):
                if step < 3 or way == m:
                    b_go(way, step, m)

    def swap(ref):
        go(ref, ref, CORES, wdr.at[0], sibling)

    pl.loop(0, 2)(states_of)
    pl.semaphore_wait(barrier, len(peers))
    send_states(0)
    send_states(1)
    done(load_sem.at[3], w_hbm)
    for k, d in enumerate((1, -1, 2, -2)):
        a_send(0, 0, d)
    own_b = wf.at[z, x, c, B]
    go(own_b, own_b, B_X, br.at[7], at_x(1))
    go(own_b, own_b, B_X, br.at[7], at_x(-1))
    done(load_sem.at[4], fb)
    states_of(2)
    send_states(2)
    states_of(3)
    send_states(3)
    done(load_sem.at[5], mix.at[pl.ds(0, 2)])
    done(load_sem.at[6], hgain_ref)
    scores_of(0)
    send_totals(0)
    send_totals(1)
    scores_of(1)
    send_totals(2)
    send_totals(3)
    scores_of(2)
    send_carried(0)
    send_carried(1)
    done(br.at[7], wf.at[pl.ds(0, 2), 0, 0, B])
    ref = wf.at[z, wrap_x(-1), c, pl.ds(32, 16)]
    go(ref, ref, B_X, br.at[8], at_x(1))
    ref = wf.at[z, wrap_x(1), c, pl.ds(48, 16)]
    go(ref, ref, B_X, br.at[8], at_x(-1))
    done(ar.at[0], wf.at[pl.ds(0, 4), 0, 0, A])
    a_send(1, -2, 1)
    a_send(1, 2, -1)
    a_send(1, -away, away)
    for k in range(3):
        a_out(k)
    scores_of(3)
    finish(0)
    done(br.at[8], wf.at[0, 0, 0, pl.ds(0, 32)])
    b_send(0)
    finish(1)
    send_carried(2)
    send_carried(3)
    for k in range(3, 5):
        a_out(k)
    a_forward(0)
    finish(2)
    finish(3)

    done(ar.at[1], wf.at[pl.ds(0, 3), 0, 0, A])
    for k in range(5, 8):
        a_out(k)
    b_send(1)
    for k in (0, -1, 1):
        swap(wf.at[wrap_z(k), :, c, B])
    a_forward(1)
    b_send(2)
    for k in (-2, 2):
        swap(wf.at[wrap_z(k), :, c, B])
    a_forward(2)
    HALVES = (pl.ds(0, TOK // 2), pl.ds(TOK // 2, TOK // 2))

    def y_forward(j):
        part = pl.ds(j * PAIR, PAIR)
        done(yr.at[j], mix.at[pl.ds(1, 2), :, part])
        d = 1 if j % 2 == 0 else -1
        source = 1 if d == 1 else 2
        for m, half in enumerate(HALVES):
            sem = yfr.at[0 if j < 2 else 1 + m]
            go(mix.at[source, half, part], mix.at[3, half, part], OVER_Y, sem, at_y(d))

    y_forward(0)
    y_forward(1)
    b_send(3)
    for k in (-3, 3):
        swap(wf.at[wrap_z(k), :, c, B])
    done(ar.at[5], wf.at[:, 0, 0, A])
    for m in range(2):
        swap(wf.at[pl.ds(4 * m, 4), :, c, A])
    y_forward(2)
    y_forward(3)
    done(br.at[6], wf.at[pl.ds(0, 2), pl.ds(0, 2), 0, B])
    swap(wf.at[wrap_z(4), :, c, B])
    done(wdr.at[0], wf.at[:, :, 0])

    def multiply(slot, place, m=None, rows_=pl.ds(0, TOK)):
        first = 2 * lax.rem(y + place + NY, NY)
        depth = COLS if m is None else COLS // 2
        left = pl.ds(0 if m is None else m * depth, depth)

        for n in range(COLS // 256):
            cols = pl.ds(n * 256, 256)
            if m is None:
                weights = wf[pl.ds(first, 2), :, :, :, cols].reshape(depth, 256)
            else:
                weights = wf[first + m, :, :, :, cols].reshape(depth, 256)
            product = dot(mix[slot, rows_, left], weights)
            acc[rows_, cols] = product if slot == 0 else acc[rows_, cols] + product

    for slot, place in ((0, 0), (1, -1), (2, 1)):
        multiply(slot, place)
    done(yfr.at[0], mix.at[3, :, pl.ds(0, COLS // 2)])
    multiply(3, 2, 0)

    done(load_sem.at[7], bgain_ref)
    done(load_sem.at[8], resb)

    def squares_of(m):
        rows_ = HALVES[m]
        done(yfr.at[1 + m], mix.at[3, rows_, pl.ds(COLS // 2, COLS // 2)])
        multiply(3, 2, 1, rows_)
        part = jnp.zeros((8, TOK // 2), F32)
        ones = jnp.ones((8, 256), BF16)
        for n in range(COLS // 256):
            cols = slice(n * 256, (n + 1) * 256)
            branch = acc[rows_, cols].astype(BF16)
            branch_buf[rows_, cols] = branch
            branch = branch.astype(F32)
            high, low = split2(branch * branch)
            part = part + dot(ones, high, NT) + dot(ones, low, NT)
        sq_send[m] = part
        for d in range(1, NY):
            go(sq_send.at[m], sq_recv.at[m, d], SQUARES, qr_.at[m], at_y(d))

    def write(m):
        rows_ = HALVES[m]
        done(qr_.at[m], sq_recv.at[m, pl.ds(1, NY - 1)])
        part = sq_send[m]
        for d in range(1, NY):
            part = part + sq_recv[m, d]
        scale = lax.rsqrt(part * (1.0 / D) + EPS)
        hi, mid, lo = split3(scale)
        parts = jnp.concatenate([hi, mid, lo, jnp.zeros_like(lo)], axis=0).astype(BF16)
        pick = lax.broadcasted_iota(jnp.int32, (32, HEAD_DIM), 0)
        pick = jnp.where(lax.rem(pick, 8) == 0, 1.0, 0.0).astype(BF16)
        column = dot(parts, pick, TN)
        for h in range(HEADS):
            cols = slice(h * HEAD_DIM, (h + 1) * HEAD_DIM)
            out_ref[rows_, cols] = (
                resb[rows_, cols].astype(F32) + branch_buf[rows_, cols].astype(F32) * column * bgain_ref[y * HEADS + h]
            ).astype(BF16)

    squares_of(0)
    squares_of(1)
    write(0)
    write(1)
    done(PHASE1, recv1.at[:, pl.ds(1, ROW - 1)])
    done(PHASE2, recv2.at[:, pl.ds(1, NZ - 1)])
    done(PHASE3, recv3.at[:, pl.ds(1, ROW - 1)])
    done(OVER_Y, mix.at[pl.ds(1, 3)])
    done(A_Z, wf.at[pl.ds(0, 7), 0, 0, A])
    done(A_X, wf.at[:, pl.ds(0, 3), 0, A])
    done(B_X, wf.at[pl.ds(0, 3), 0, 0, A])
    done(B_Z, wf.at[pl.ds(0, 7), :, 0, B])
    done(CORES, wf.at[:, :, 0])
    done(SQUARES, sq_recv.at[:, pl.ds(1, NY - 1)])


def per_device(q, f, v, g, gap, surge, hgain, w, bgain, res):
    any_ = pl.BlockSpec(memory_space=pltpu.HBM)
    vmem = pl.BlockSpec(memory_space=pltpu.VMEM)
    dma = pltpu.SemaphoreType.DMA
    block = (TOK, COLS)
    state = (PART, HEAD_DIM)
    message = (PART + 16, HEAD_DIM)
    scratch = [
        pltpu.VMEM(block, BF16),
        pltpu.VMEM(block, BF16),
        pltpu.VMEM(block, BF16),
        pltpu.VMEM(block, BF16),
        pltpu.VMEM(block, BF16),
        pltpu.VMEM(block, BF16),
        pltpu.VMEM((NY * HEADS // 2, 1, PAIR), F32),
        pltpu.VMEM((HEADS, TOK), F32),
        pltpu.VMEM((1, HEAD_DIM), F32),
        pltpu.VMEM((NY * HEADS, 1, HEAD_DIM), F32),
        pltpu.VMEM((NZ, NX, NC, 64, COLS), BF16),
        pltpu.VMEM((NY,) + block, BF16),
        pltpu.VMEM(block, F32),
        pltpu.VMEM(block, BF16),
        pltpu.VMEM(block, BF16),
        pltpu.VMEM(block, F32),
        pltpu.VMEM(block, F32),
        pltpu.VMEM((HEADS, CHUNKS, HEAD_DIM, HEAD_DIM), F32),
        pltpu.VMEM((HEADS // 2, CHUNKS, 8, PAIR), F32),
        pltpu.VMEM((CHUNK, 2 * CHUNK), BF16),
        pltpu.VMEM((32, TOK), BF16),
        pltpu.VMEM((GROUPS, ROW) + message, BF16),
        pltpu.VMEM((GROUPS, ROW) + message, BF16),
        pltpu.VMEM((GROUPS, ROW) + state, F32),
        pltpu.VMEM((GROUPS, ROW, 1, HEAD_DIM), F32),
        pltpu.VMEM((GROUPS,) + message, BF16),
        pltpu.VMEM((GROUPS, NZ) + message, BF16),
        pltpu.VMEM((GROUPS, ROW) + state, BF16),
        pltpu.VMEM((GROUPS, ROW) + state, BF16),
        pltpu.VMEM((2, 8, TOK // 2), F32),
        pltpu.VMEM((2, NY, 8, TOK // 2), F32),
        pltpu.VMEM(block, F32),
        dma((9,)),
        dma((10,)),
        dma((GROUPS,)), dma((GROUPS,)), dma((GROUPS,)), dma((4,)), dma((3,)), dma((6,)), dma((9,)), dma((1,)), dma((2,)),
    ]
    return pl.pallas_call(
        kernel,
        out_shape=pltpu.VMEM(block, BF16),
        in_specs=[any_] * 10,
        out_specs=vmem,
        scratch_shapes=scratch,
        compiler_params=pltpu.CompilerParams(
            collective_id=0, has_side_effects=True, vmem_limit_bytes=VMEM_LIMIT
        ),
    )(
        q, f, v, g, w, res,
        gap.reshape(NY * HEADS // 2, 1, PAIR), surge, hgain.reshape(1, HEAD_DIM),
        bgain.reshape(NY * HEADS, 1, HEAD_DIM),
    )


def solution(mesh):
    torus = Mesh(mesh.devices.reshape(NZ, NX, NC, NY), ("z", "x", "c", "y"))
    cut = P(SP, "y")
    in_specs = (cut, cut, cut, cut, P(), P("y", SP), P(), cut, P(), cut)
    return jax.shard_map(per_device, mesh=torus, in_specs=in_specs, out_specs=cut, check_vma=False)
```
